32 devices in a mesh: sp: 4 (over z), fs: 4 (over y, x), tp: 2 (over core).
Axes of the slice: x: 2, y: 2, z: 4, core: 2. Of those that a mesh axis runs over, the one named last changes fastest.
Arguments:
- queries: bfloat16 [4, 1024, 512], P('fs', 'sp', 'tp'), may hold values from -60 to 60
- keys: bfloat16 [4, 1024, 256], P('fs', 'sp', 'tp'), may hold values from -4.5 to 4.5
- values: bfloat16 [4, 1024, 256], P('fs', 'sp', 'tp'), may hold values from -6 to 6
- forget_cache: float32 [4, 1024, 8], P('fs', 'sp', 'tp'), may hold values from -128 to 0, as said below
- fox_gain: float32 [512], P('tp'), may hold values from 0.1 to 1.9
- receptance: bfloat16 [4, 1024, 512], P('fs', 'sp', 'tp'), may hold values from -6 to 6
- lin_keys: bfloat16 [4, 1024, 512], P('fs', 'sp', 'tp'), may hold values from -6 to 6
- lin_values: bfloat16 [4, 1024, 512], P('fs', 'sp', 'tp'), may hold values from -6 to 6
- learn_logit: bfloat16 [4, 1024, 512], P('fs', 'sp', 'tp'), may hold values from -12 to 4
- decay_log: float32 [4, 1024, 512], P('fs', 'sp', 'tp'), may hold values from -16 to 0
- lin_gain: float32 [512], P('tp'), may hold values from 0.1 to 1.9
- out_fox_weight: bfloat16 [512, 2048], P('tp', 'fs'), may hold values from -0.1875 to 0.1875
- out_lin_weight: bfloat16 [512, 2048], P('tp', 'fs'), may hold values from -0.1875 to 0.1875
Outputs:
- mixed: bfloat16 [4, 1024, 2048], P('fs', ('sp', 'tp'))
The draws below stay inside these ranges and needn't reach their ends.
Inputs may be any that keep to these rules, and one draw needn't show every extreme that they name: `forget_cache`: Non-increasing along the positions of each sequence and head.
All inputs are finite; a program needn't handle non-finite values.
Results may differ from the reference program's by a relative error of at most 0.017.
Values may be sent and summed in bfloat16 or wider, within the bound.
A program may use at most 64 MiB of HBM per device.

```python
import math
import jax
import jax.numpy as jnp
from jax import lax

D = 2048
HEAD = 64
FOX_HEADS = 8
KEY_HEADS = 4
LIN_HEADS = 8
TOK_DEV = 256
W_FOX = 512
W_LIN = 512
SEQUENCE_COUNT = 4
SEQUENCE_LENGTH = 1024
N_TP = 2


def slow_flags(key, salt, count):
    order = jax.random.permutation(jax.random.fold_in(key, salt), count)
    return order < count // 2


def lin_flags(key):
    return jnp.repeat(slow_flags(key, 5, LIN_HEADS), HEAD)


def step_rates(key, salt, count, slow_heads):
    split_keys = jax.random.split(jax.random.fold_in(key, salt), 6)
    chain_total = jax.random.uniform(split_keys[0], (SEQUENCE_COUNT, 1, count), jnp.float32, 0.15, 0.5)
    reach_steps = jax.random.uniform(split_keys[1], (SEQUENCE_COUNT, 1, count), jnp.float32, 30.0, 100.0)
    baseline_rate = jnp.where(slow_heads[None, None, :], chain_total / SEQUENCE_LENGTH, 1.0 / reach_steps)
    block_list = jnp.exp(jax.random.uniform(split_keys[2], (SEQUENCE_COUNT, SEQUENCE_LENGTH // TOK_DEV, 1), jnp.float32, -0.7, 0.7))
    block_list = jnp.repeat(block_list, TOK_DEV, axis=1)
    nearby_factor = jax.random.uniform(split_keys[3], (SEQUENCE_COUNT, SEQUENCE_LENGTH, count), jnp.float32, 0.3, 1.7)
    spurt_rows = jax.random.randint(split_keys[4], (SEQUENCE_COUNT, 3), 0, SEQUENCE_LENGTH)
    spurt_depth = jax.random.uniform(split_keys[5], (SEQUENCE_COUNT, 3), jnp.float32, 0.22, 0.5)
    matched_rows = (jnp.arange(SEQUENCE_LENGTH)[None, :, None] == spurt_rows[:, None, :]).astype(jnp.float32)
    spurt_groups = jnp.sum(matched_rows * spurt_depth[:, None, :], axis=-1)
    gradual_float = slow_heads.astype(jnp.float32)
    return baseline_rate * block_list * nearby_factor + spurt_groups[:, :, None] * gradual_float[None, None, :]


def query_key(key):
    split_keys = jax.random.split(jax.random.fold_in(key, 7), 2)
    key_float = jnp.clip(jax.random.normal(split_keys[0], (SEQUENCE_COUNT, SEQUENCE_LENGTH, KEY_HEADS * HEAD), jnp.float32), -4.5, 4.5)
    query_float = jnp.clip(1.5 * jax.random.normal(split_keys[1], (SEQUENCE_COUNT, SEQUENCE_LENGTH, FOX_HEADS * HEAD), jnp.float32), -9.0, 9.0)
    return (query_float, key_float)


def draw_queries(key, part):
    return query_key(key)[0].astype(jnp.bfloat16)


def draw_keys(key, part):
    return query_key(key)[1].astype(jnp.bfloat16)


def draw_forget_cache(key, part):
    slow_heads = slow_flags(key, 3, FOX_HEADS)
    rates = step_rates(key, 13, FOX_HEADS, slow_heads)
    return -jnp.cumsum(rates, axis=1)


def draw_decay_log(key, part):
    slow_heads = lin_flags(key)
    return jnp.log(step_rates(key, 17, LIN_HEADS * HEAD, slow_heads))


def draw_learn_logit(key, part):
    slow_heads = lin_flags(key)
    noise_key = jax.random.fold_in(key, 23)
    spread = jnp.clip(jax.random.normal(noise_key, (SEQUENCE_COUNT, SEQUENCE_LENGTH, LIN_HEADS * HEAD), jnp.float32), -4.0, 4.0)
    return (spread - 8.0 * slow_heads.astype(jnp.float32)[None, None, :]).astype(jnp.bfloat16)


def shard_levels(key, shape, cuts, least, high):
    loudness = 1.0
    for position, parts in cuts:
        steps = jax.random.uniform(jax.random.fold_in(jax.random.fold_in(key, 6), position), (parts,), jnp.float32, least / len(cuts), high / len(cuts))
        loudness = loudness * jnp.repeat(jnp.exp(steps), shape[position] // parts).reshape((-1,) + (1,) * (len(shape) - 1 - position))
    return loudness


def bell_draw(key, shape, scale, bound, cuts=(), held_as=jnp.bfloat16):
    drawn = jax.random.normal(key, shape, jnp.float32) * scale
    if len(cuts) > 0:
        drawn = shard_levels(key, shape, cuts, -0.22, 0.18) * drawn
    return jnp.clip(drawn, min=-bound, max=bound).astype(held_as)


def setup_inputs(seed: int = 0) -> dict:
    key_of = jax.random.split(jax.random.key(seed), 14)
    return {
        "queries": draw_queries(jax.random.fold_in(key_of[13], 71), 0),
        "keys": draw_keys(jax.random.fold_in(key_of[13], 71), 0),
        "values": bell_draw(key_of[2], (SEQUENCE_COUNT, SEQUENCE_LENGTH, KEY_HEADS * HEAD), 1.0, 6.0, ((0, 4), (1, 4), (2, 2))),
        "forget_cache": draw_forget_cache(jax.random.fold_in(key_of[13], 71), 0),
        "fox_gain": jnp.clip(1.0 + 0.18 * jax.random.normal(key_of[4], (W_FOX,), jnp.float32), 0.1, 1.9),
        "receptance": bell_draw(key_of[5], (SEQUENCE_COUNT, SEQUENCE_LENGTH, W_LIN), 1.0, 6.0, ((0, 4), (1, 4), (2, 2))),
        "lin_keys": bell_draw(key_of[6], (SEQUENCE_COUNT, SEQUENCE_LENGTH, W_LIN), 1.0, 6.0, ((0, 4), (1, 4), (2, 2))),
        "lin_values": bell_draw(key_of[7], (SEQUENCE_COUNT, SEQUENCE_LENGTH, W_LIN), 1.0, 6.0, ((0, 4), (1, 4), (2, 2))),
        "learn_logit": draw_learn_logit(jax.random.fold_in(key_of[13], 71), 0),
        "decay_log": draw_decay_log(jax.random.fold_in(key_of[13], 71), 0),
        "lin_gain": jnp.clip(1.0 + 0.18 * jax.random.normal(key_of[10], (W_LIN,), jnp.float32), 0.1, 1.9),
        "out_fox_weight": bell_draw(key_of[11], (W_FOX, D), (W_FOX + W_LIN) ** -0.5, 0.1875, ((0, 2), (1, 4))),
        "out_lin_weight": bell_draw(key_of[12], (W_LIN, D), (W_FOX + W_LIN) ** -0.5, 0.1875, ((0, 2), (1, 4))),
    }


HIGHEST = lax.Precision.HIGHEST
NORM_EPS = 1e-06

def round_half(tensor):
    return lax.optimization_barrier(tensor.astype(jnp.bfloat16)).astype(jnp.float32)

def forget_attention(query_rows, key_rows, value_rows, forget_rows, fox_gain):
    length = query_rows.shape[0]
    group_size = FOX_HEADS // KEY_HEADS
    block_rows = math.gcd(length, 512)
    block_count = length // block_rows
    score_scale = HEAD ** (-0.5)
    query_all = query_rows.astype(jnp.float32).reshape(block_count, block_rows, KEY_HEADS, group_size, HEAD)
    key_all = key_rows.astype(jnp.float32).reshape(block_count, block_rows, KEY_HEADS, HEAD)
    value_all = value_rows.astype(jnp.float32).reshape(block_count, block_rows, KEY_HEADS, HEAD)
    forget_all = jnp.transpose(forget_rows.reshape(block_count, block_rows, KEY_HEADS, group_size), (0, 2, 3, 1))
    offsets = jnp.arange(block_rows, dtype=jnp.int32)

    def query_block(block_index):
        query_here = query_all[block_index]
        forget_here = forget_all[block_index]

        def key_block(other, running):
            running_max, totals, weighted = running
            scores = jnp.einsum('tkgd,skd->kgts', query_here, key_all[other], precision=HIGHEST) * score_scale
            scores = scores + forget_here[:, :, :, None] - forget_all[other][:, :, None, :]
            allowed = (other * block_rows + offsets)[None, :] <= (block_index * block_rows + offsets)[:, None]
            scores = jnp.where(allowed, scores, -jnp.inf)
            new_max = jnp.maximum(running_max, lax.optimization_barrier(jnp.max(scores, axis=-1)))
            rescale = jnp.exp(running_max - new_max)
            weights = jnp.exp(scores - new_max[..., None])
            totals = totals * rescale + lax.optimization_barrier(jnp.sum(weights, axis=-1))
            update = jnp.einsum('kgts,skd->kgtd', round_half(weights), value_all[other], precision=HIGHEST)
            weighted = weighted * rescale[..., None] + update
            return (new_max, totals, weighted)
        start_state = (jnp.full((KEY_HEADS, group_size, block_rows), -jnp.inf, jnp.float32), jnp.zeros((KEY_HEADS, group_size, block_rows), jnp.float32), jnp.zeros((KEY_HEADS, group_size, block_rows, HEAD), jnp.float32))
        running_max, totals, weighted = lax.fori_loop(0, block_index + 1, key_block, start_state)
        heads_out = weighted / totals[..., None]
        return jnp.transpose(heads_out, (2, 0, 1, 3)).reshape(block_rows, FOX_HEADS, HEAD)
    attended = lax.map(query_block, jnp.arange(block_count, dtype=jnp.int32)).reshape(length, FOX_HEADS, HEAD)
    normed = attended * lax.rsqrt(lax.optimization_barrier(jnp.mean(attended * attended, axis=-1, keepdims=True)) + NORM_EPS)
    return (normed * fox_gain.reshape(FOX_HEADS, HEAD)).reshape(length, W_FOX).astype(jnp.bfloat16)

def delta_attention(recept_rows, key_rows, value_rows, learn_rows, decay_rows, lin_gain):
    length = recept_rows.shape[0]
    head_shape = (length, LIN_HEADS, HEAD)
    recept_float = recept_rows.astype(jnp.float32).reshape(head_shape)
    key_float = key_rows.astype(jnp.float32).reshape(head_shape)
    value_float = value_rows.astype(jnp.float32).reshape(head_shape)
    learn_rate = jax.nn.sigmoid(learn_rows.astype(jnp.float32)).reshape(head_shape)
    unit_keys = key_float * lax.rsqrt(lax.optimization_barrier(jnp.sum(key_float * key_float, axis=-1, keepdims=True)) + NORM_EPS)
    decays = jnp.exp(-jnp.exp(decay_rows)).reshape(head_shape)

    def advance(state, inputs):
        recept_t, key_t, value_t, unit_t, rate_t, decay_t = inputs
        projected = jnp.einsum('hvk,hk->hv', state, unit_t, precision=HIGHEST)
        state = state * decay_t[:, None, :] - projected[:, :, None] * (unit_t * rate_t)[:, None, :] + value_t[:, :, None] * key_t[:, None, :]
        return (state, jnp.einsum('hvk,hk->hv', state, recept_t, precision=HIGHEST))
    start_state = jnp.zeros((LIN_HEADS, HEAD, HEAD), jnp.float32)
    _, readout = lax.scan(advance, start_state, (recept_float, key_float, value_float, unit_keys, learn_rate, decays))
    centred = readout - lax.optimization_barrier(jnp.mean(readout, axis=-1, keepdims=True))
    normed = centred * lax.rsqrt(lax.optimization_barrier(jnp.mean(centred * centred, axis=-1, keepdims=True)) + HEAD * 1e-05)
    return (normed * lin_gain.reshape(LIN_HEADS, HEAD)).reshape(length, W_LIN).astype(jnp.bfloat16)

def reference(queries, keys, values, forget_cache, fox_gain, receptance, lin_keys, lin_values, learn_logit, decay_log, lin_gain, out_fox_weight, out_lin_weight):
    fox_part = W_FOX // N_TP
    lin_part = W_LIN // N_TP

    def one_sequence(inputs):
        query_rows, key_rows, value_rows, forget_rows, recept_rows, lkey_rows, lvalue_rows, learn_rows, decay_rows = inputs
        fox_out = forget_attention(query_rows, key_rows, value_rows, forget_rows, fox_gain)
        lin_out = delta_attention(recept_rows, lkey_rows, lvalue_rows, learn_rows, decay_rows, lin_gain)
        mixed = jnp.zeros((fox_out.shape[0], D), jnp.float32)
        for slot_index in range(N_TP):
            fox_cols = slice(slot_index * fox_part, (slot_index + 1) * fox_part)
            lin_cols = slice(slot_index * lin_part, (slot_index + 1) * lin_part)
            partial_value = jnp.dot(fox_out[:, fox_cols], out_fox_weight[fox_cols], preferred_element_type=jnp.float32)
            partial_value = partial_value + jnp.dot(lin_out[:, lin_cols], out_lin_weight[lin_cols], preferred_element_type=jnp.float32)
            mixed = mixed + round_half(partial_value)
        return mixed.astype(jnp.bfloat16)
    return lax.map(one_sequence, (queries, keys, values, forget_cache, receptance, lin_keys, lin_values, learn_logit, decay_log))
```

```python
import functools

import jax
import jax.numpy as jnp
from jax import lax
from jax.experimental import pallas as pl
from jax.experimental.pallas import tpu as pltpu
from jax.sharding import PartitionSpec as P

HEAD = 64
SPAN = 64
SPAN_BITS = SPAN.bit_length() - 1
NORM_EPS = 1e-06
MESH = pl.DeviceIdType.MESH
F32 = jnp.float32
BF16 = jnp.bfloat16


def pieces(x, count):
    out = []
    for _ in range(count - 1):
        top = x.astype(BF16)
        out.append(top)
        x = x - top.astype(F32)
    out.append(x.astype(BF16))
    return out


def dot(a, b, dims, passes):
    run = functools.partial(lax.dot_general, dimension_numbers=dims, preferred_element_type=F32)
    if passes == 1:
        return run(a.astype(BF16), b.astype(BF16))
    a_hi, a_lo = pieces(a, 2)
    if passes == 2:
        return run(a_hi, b.astype(BF16)) + run(a_lo, b.astype(BF16))
    b_hi, b_lo = pieces(b, 2)
    return run(a_hi, b_hi) + (run(a_hi, b_lo) + run(a_lo, b_hi))


NN = (((1,), (0,)), ((), ()))
NT = (((1,), (1,)), ((), ()))
BNN = (((2,), (1,)), ((0,), (0,)))
BNT = (((2,), (2,)), ((0,), (0,)))


def iota(shape, dim):
    return lax.broadcasted_iota(jnp.int32, shape, dim)


def delta_maps(recept, keys, values, learn, decay_log, passes):
    rows, width = recept.shape
    spans, heads = rows // SPAN, width // HEAD
    i, j = iota((rows, rows), 0), iota((rows, rows), 1)
    lower = ((i >> SPAN_BITS) == (j >> SPAN_BITS)) & (j <= i)
    lower = jnp.where(lower, 1.0, 0.0).astype(BF16)
    ones = head_ones(width)
    keys, values, recept = keys.astype(F32), values.astype(F32), recept.astype(F32)
    rate = jax.nn.sigmoid(learn.astype(F32))
    unit = keys * lax.rsqrt(dot(keys * keys, ones, NN, 2) + NORM_EPS)
    fall = -jnp.exp(decay_log)
    inclusive = sum(
        lax.dot_general(lower, part, NN, preferred_element_type=F32) for part in pieces(fall, 3)
    )
    last = jnp.concatenate(
        [
            jnp.broadcast_to(inclusive[(c + 1) * SPAN - 1 : (c + 1) * SPAN], (SPAN, width))
            for c in range(spans)
        ],
        axis=0,
    )
    shrunk = jnp.exp(-inclusive)
    tail = jnp.exp(last - inclusive)
    unit_rate = unit * rate

    def cut(x):
        return jnp.stack(
            [
                x[c * SPAN : (c + 1) * SPAN, h * HEAD : (h + 1) * HEAD]
                for c in range(spans)
                for h in range(heads)
            ]
        )

    def cut_turned(x):
        x = jnp.transpose(x)
        return jnp.stack(
            [
                x[h * HEAD : (h + 1) * HEAD, c * SPAN : (c + 1) * SPAN]
                for c in range(spans)
                for h in range(heads)
            ]
        )

    erase_in = cut(-unit * jnp.exp(inclusive - fall))
    read_in = cut(recept * jnp.exp(inclusive))
    erase_out, write_out = cut(unit_rate * shrunk), cut(keys * shrunk)
    value = cut(values)
    count = spans * heads
    zero = jnp.zeros((count, SPAN, HEAD), F32)

    i, j = iota((2 * SPAN, 2 * SPAN), 0), iota((2 * SPAN, 2 * SPAN), 1)
    allowed = (j & (SPAN - 1)) < (i & (SPAN - 1)) + (i >> SPAN_BITS)
    mixes = dot(
        jnp.concatenate([erase_in, read_in], 1),
        jnp.concatenate([erase_out, write_out], 1),
        BNT,
        passes,
    )
    mixes = jnp.where(allowed[None], mixes, 0.0)
    erase = mixes[:, :SPAN, :SPAN]
    i, j = iota((SPAN, SPAN), 0), iota((SPAN, SPAN), 1)

    def level(bit):
        same = (i >> (bit + 1)) == (j >> (bit + 1))
        return (same & (((i >> bit) & 1) == 1) & (((j >> bit) & 1) == 0))[None]

    inverse = jnp.where((i == j)[None], 1.0, jnp.where(level(0), erase, 0.0))
    for bit in range(1, SPAN_BITS):
        step = jnp.where(level(bit), erase, 0.0)
        inverse = inverse + dot(inverse, dot(step, inverse, BNN, passes), BNN, passes)
    mixed_values = dot(mixes, jnp.concatenate([zero, value], 1), BNN, passes)
    erased = dot(
        inverse, jnp.concatenate([erase_in, mixed_values[:, :SPAN]], 2), BNN, passes
    )
    outs = jnp.concatenate([read_in, mixed_values[:, SPAN:]], 2) + dot(
        mixes[:, SPAN:, :SPAN], erased, BNN, passes
    )
    turned = jnp.concatenate([cut_turned(unit_rate * tail), cut_turned(keys * tail)], 2)
    grow = jnp.exp(last)
    grow = jnp.concatenate([cut(grow), zero], 2)
    i, j = iota((HEAD, 2 * HEAD), 0), iota((HEAD, 2 * HEAD), 1)
    maps = dot(
        turned,
        jnp.concatenate([erased, jnp.concatenate([zero, value], 2)], 1),
        BNN,
        passes,
    ) + jnp.where((i == j)[None], grow, 0.0)
    right = (j >= HEAD)[None]
    before = maps[:heads]
    carried = [outs[:heads]]
    for c in range(1, spans):
        here = slice(c * heads, (c + 1) * heads)
        carried.append(
            dot(outs[here][:, :, :HEAD], before, BNN, passes) + jnp.where(right, outs[here], 0.0)
        )
        before = dot(maps[here][:, :, :HEAD], before, BNN, passes) + jnp.where(
            right, maps[here], 0.0
        )
    return jnp.concatenate(carried, 0), before


def head_ones(width):
    bits = HEAD.bit_length() - 1
    i, j = iota((width, width), 0), iota((width, width), 1)
    return jnp.where((i >> bits) == (j >> bits), 1.0, 0.0).astype(BF16)


def kernel(
    sizes, passes,
    q_ref, k_ref, v_ref, f_ref, fox_gain_ref,
    r_ref, lk_ref, lv_ref, learn_ref, decay_ref, lin_gain_ref,
    wf_ref, wl_ref,
    out_ref,
    k_buf, v_buf, f_buf, map_own, map_buf, w_buf, carried_ref,
    max_ref, total_ref, acc_ref, act_ref, part_own, part_buf,
    k_send, v_send, f_send, k_recv, v_recv, f_recv,
    map_send, map_recv, w_send, w_recv, part_send, part_recv, local_sem,
):
    n_sp, n_fs, n_tp = sizes
    me, fs, tp = lax.axis_index("sp"), lax.axis_index("fs"), lax.axis_index("tp")
    rows, width = q_ref.shape
    heads = width // HEAD
    kv_heads = k_ref.shape[1] // HEAD
    group = heads // kv_heads
    lin_heads = r_ref.shape[1] // HEAD
    spans = rows // SPAN
    lin_width = r_ref.shape[1]
    block = wf_ref.shape[1]
    half = rows // n_tp

    barrier = pltpu.get_barrier_semaphore()

    def greet(step, _):
        pl.semaphore_signal(
            barrier, inc=1, device_id={"sp": lax.rem(me + step, n_sp)}, device_id_type=MESH
        )
        return 0

    lax.fori_loop(1, n_sp, greet, 0)
    for step in range(1, n_fs):
        pl.semaphore_signal(
            barrier, inc=1, device_id={"fs": lax.rem(fs + step, n_fs)}, device_id_type=MESH
        )
    for step in range(1, n_tp):
        pl.semaphore_signal(
            barrier, inc=1, device_id={"tp": lax.rem(tp + step, n_tp)}, device_id_type=MESH
        )
    pl.semaphore_wait(barrier, n_sp + n_fs + n_tp - 3)

    def to_later(src, buf, send, recv, other):
        return pltpu.make_async_remote_copy(
            src_ref=src, dst_ref=buf.at[me], send_sem=send.at[other], recv_sem=recv.at[me],
            device_id={"sp": other}, device_id_type=MESH,
        )

    def from_earlier(src, buf, send, recv, other):
        return pltpu.make_async_remote_copy(
            src_ref=src, dst_ref=buf.at[other], send_sem=send.at[other], recv_sem=recv.at[other],
            device_id={"sp": other}, device_id_type=MESH,
        )

    shared = (
        (k_ref, k_buf, k_send, k_recv),
        (v_ref, v_buf, v_send, v_recv),
        (f_ref, f_buf, f_send, f_recv),
    )

    def send_block(other, _):
        for item in shared:
            to_later(*item, other).start()
        return 0

    lax.fori_loop(me + 1, n_sp, send_block, 0)

    def weight_copy(which, step):
        src = (wf_ref, wl_ref)[which]
        return pltpu.make_async_remote_copy(
            src_ref=src, dst_ref=w_buf.at[fs, which],
            send_sem=w_send.at[which, step], recv_sem=w_recv.at[which, fs],
            device_id={"fs": lax.rem(fs + step, n_fs)}, device_id_type=MESH,
        )

    def weight_wait(which, source):
        return pltpu.make_async_remote_copy(
            src_ref=(wf_ref, wl_ref)[which], dst_ref=w_buf.at[source, which],
            send_sem=w_send.at[which, 0], recv_sem=w_recv.at[which, source],
            device_id={"fs": source}, device_id_type=MESH,
        )

    for which in range(2):
        for step in range(1, n_fs):
            weight_copy(which, step).start()
    own = [
        pltpu.make_async_copy((wf_ref, wl_ref)[which], w_buf.at[fs, which], local_sem.at[which])
        for which in range(2)
    ]
    for copy in own:
        copy.start()

    carried, maps = delta_maps(
        r_ref[...], lk_ref[...], lv_ref[...], learn_ref[...], decay_ref[...], passes
    )
    map_own[...] = maps.astype(BF16)
    carried_ref[...] = carried

    def send_map(other, _):
        to_later(map_own, map_buf, map_send, map_recv, other).start()
        return 0

    lax.fori_loop(me + 1, n_sp, send_map, 0)

    scaled = (q_ref[...].astype(F32) * HEAD ** (-0.5)).astype(BF16)

    def attend(key_block, value_block, forget_block, first):
        forget = jnp.transpose(forget_block)
        turned = jnp.transpose(value_block)
        if first:
            seen = iota((rows, rows), 0) <= iota((rows, rows), 1)
        for h in range(heads):
            kv = slice(h // group * HEAD, (h // group + 1) * HEAD)
            scores = lax.dot_general(
                key_block[:, kv], scaled[:, h * HEAD : (h + 1) * HEAD], NT,
                preferred_element_type=F32,
            ) - forget[:, h : h + 1]
            if first:
                scores = jnp.where(seen, scores, -1e30)
            top = jnp.max(scores, axis=0, keepdims=True)
            if not first:
                old = max_ref[h]
                top = jnp.maximum(old, top)
                rescale = jnp.exp(old - top)
            weights = jnp.exp(scores - top)
            total = jnp.sum(weights, axis=0, keepdims=True)
            update = lax.dot_general(
                turned[kv], weights.astype(BF16), NN, preferred_element_type=F32
            )
            if not first:
                total = total + total_ref[h] * rescale
                update = update + acc_ref[h] * rescale
            max_ref[h] = top
            total_ref[h] = total
            acc_ref[h] = update

    attend(k_ref[...], v_ref[...], f_ref[...], True)

    def earlier(step, _):
        other = me - 1 - step
        for item in shared:
            from_earlier(*item, other).wait_recv()
        attend(k_buf[other], v_buf[other], f_buf[other], False)
        return 0

    lax.fori_loop(0, me, earlier, 0)
    normed = []
    for h in range(heads):
        attended = acc_ref[h] / total_ref[h]
        normed.append(
            attended
            * lax.rsqrt(jnp.mean(attended * attended, axis=0, keepdims=True) + NORM_EPS)
        )
    fox_out = jnp.transpose(jnp.concatenate(normed, axis=0)) * fox_gain_ref[...]
    act_ref[:, :width] = fox_out.astype(BF16)

    def join(other, state):
        from_earlier(map_own, map_buf, map_send, map_recv, other).wait_recv()
        step = map_buf[other]
        return dot(step[:, :, :HEAD].astype(F32), state, BNN, passes) + step[:, :, HEAD:].astype(F32)

    state = lax.fori_loop(0, me, join, jnp.zeros((lin_heads, HEAD, HEAD), F32))
    eye = jnp.where(iota((HEAD, HEAD), 0) == iota((HEAD, HEAD), 1), 1.0, 0.0)
    eye = jnp.broadcast_to(eye[None], (lin_heads, HEAD, HEAD))
    state = jnp.concatenate([state, eye], axis=1)
    read = []
    for c in range(spans):
        here = dot(carried_ref[c * lin_heads : (c + 1) * lin_heads], state, BNN, 3)
        read.append(jnp.concatenate([here[h] for h in range(lin_heads)], axis=1))
    read = jnp.concatenate(read, axis=0)
    ones = head_ones(lin_width)
    centred = read - dot(read, ones, NN, 2) * (1.0 / HEAD)
    spread = dot(centred * centred, ones, NN, 2) * (1.0 / HEAD)
    lin_out = centred * lax.rsqrt(spread + HEAD * 1e-05) * lin_gain_ref[...]
    act_ref[:, width:] = lin_out.astype(BF16)

    def project(first, source):
        act = act_ref[pl.ds(pl.multiple_of(first, half), half), :]
        return lax.dot_general(
            act[:, :width], w_buf[source, 0], NN, preferred_element_type=F32
        ) + lax.dot_general(act[:, width:], w_buf[source, 1], NN, preferred_element_type=F32)

    def part_copy(step, source):
        return pltpu.make_async_remote_copy(
            src_ref=part_own.at[step - 1, source], dst_ref=part_buf.at[step - 1, source],
            send_sem=part_send.at[step - 1, source], recv_sem=part_recv.at[step - 1, source],
            device_id={"tp": lax.rem(tp + step, n_tp)}, device_id_type=MESH,
        )

    for copy in own:
        copy.wait()
    for hop in range(n_fs):
        source = lax.rem(fs + hop, n_fs)
        if hop > 0:
            for which in range(2):
                weight_wait(which, source).wait_recv()
        for step in range(1, n_tp):
            part_own[step - 1, source] = project(
                lax.rem(tp + step, n_tp) * half, source
            ).astype(BF16)
            part_copy(step, source).start()
    for source in range(n_fs):
        total = project(tp * half, source).astype(BF16).astype(F32)
        for step in range(1, n_tp):
            part_copy(step, source).wait_recv()
            total = total + part_buf[step - 1, source].astype(F32)
        out_ref[:, source * block : (source + 1) * block] = total.astype(BF16)

    def drain(other, _):
        for item in shared + ((map_own, map_buf, map_send, map_recv),):
            to_later(*item, other).wait_send()
        return 0

    lax.fori_loop(me + 1, n_sp, drain, 0)
    for which in range(2):
        for step in range(1, n_fs):
            weight_copy(which, step).wait_send()
    for source in range(n_fs):
        for step in range(1, n_tp):
            part_copy(step, source).wait_send()


def shards(
    sizes, passes,
    queries, keys, values, forget_cache, fox_gain, receptance, lin_keys, lin_values,
    learn_logit, decay_log, lin_gain, out_fox_weight, out_lin_weight,
):
    n_sp, n_fs, n_tp = sizes
    _, rows, width = queries.shape
    kv_width = keys.shape[2]
    lin_width = receptance.shape[2]
    heads, lin_heads = width // HEAD, lin_width // HEAD
    fox_rows, block = out_fox_weight.shape
    half = rows // n_tp
    forget = jnp.transpose(forget_cache[0])
    forget = jnp.pad(forget, ((0, -forget.shape[0] % 8), (0, 0)))
    dma = pltpu.SemaphoreType.DMA
    vmem = pltpu.VMEM
    out = pl.pallas_call(
        functools.partial(kernel, sizes, passes),
        out_shape=jax.ShapeDtypeStruct((half, n_fs * block), BF16),
        in_specs=[pl.BlockSpec(memory_space=vmem)] * 13,
        out_specs=pl.BlockSpec(memory_space=vmem),
        scratch_shapes=[
            vmem((n_sp, rows, kv_width), BF16),
            vmem((n_sp, rows, kv_width), BF16),
            vmem((n_sp,) + forget.shape, F32),
            vmem((lin_heads, HEAD, 2 * HEAD), BF16),
            vmem((n_sp, lin_heads, HEAD, 2 * HEAD), BF16),
            vmem((n_fs, 2, fox_rows, block), BF16),
            vmem((rows // SPAN * lin_heads, SPAN, 2 * HEAD), F32),
            vmem((heads, 1, rows), F32),
            vmem((heads, 1, rows), F32),
            vmem((heads, HEAD, rows), F32),
            vmem((rows, width + lin_width), BF16),
            vmem((n_tp - 1, n_fs, half, block), BF16),
            vmem((n_tp - 1, n_fs, half, block), BF16),
        ]
        + [dma((n_sp,))] * 8
        + [dma((2, n_fs))] * 2
        + [dma((n_tp - 1, n_fs))] * 2
        + [dma((2,))],
        compiler_params=pltpu.CompilerParams(
            collective_id=0, has_side_effects=True, vmem_limit_bytes=60 * 1024 * 1024
        ),
    )(
        queries[0], keys[0], values[0], forget, fox_gain[None],
        receptance[0], lin_keys[0], lin_values[0], learn_logit[0], decay_log[0], lin_gain[None],
        out_fox_weight, out_lin_weight,
    )
    return out[None]


def solution(mesh, passes=3):
    sizes = tuple(mesh.shape[name] for name in ("sp", "fs", "tp"))
    rows = P("fs", "sp", "tp")
    return jax.shard_map(
        functools.partial(shards, sizes, passes),
        mesh=mesh,
        in_specs=(rows,) * 4 + (P("tp"),) + (rows,) * 5 + (P("tp"), P("tp", "fs"), P("tp", "fs")),
        out_specs=P("fs", ("sp", "tp"), None),
        check_vma=False,
    )
```

```python
import functools

import jax
import jax.numpy as jnp
from jax import lax
from jax.experimental import pallas as pl
from jax.experimental.pallas import tpu as pltpu
from jax.sharding import PartitionSpec as P

HEAD = 64
SPAN = 64
SPAN_BITS = SPAN.bit_length() - 1
NORM_EPS = 1e-06
MESH = pl.DeviceIdType.MESH
F32 = jnp.float32
BF16 = jnp.bfloat16


def pieces(x, count):
    out = []
    for _ in range(count - 1):
        top = x.astype(BF16)
        out.append(top)
        x = x - top.astype(F32)
    out.append(x.astype(BF16))
    return out


def dot(a, b, dims, passes):
    run = functools.partial(lax.dot_general, dimension_numbers=dims, preferred_element_type=F32)
    if passes == 1:
        return run(a.astype(BF16), b.astype(BF16))
    a_hi, a_lo = pieces(a, 2)
    if passes == 2:
        return run(a_hi, b.astype(BF16)) + run(a_lo, b.astype(BF16))
    b_hi, b_lo = pieces(b, 2)
    return run(a_hi, b_hi) + (run(a_hi, b_lo) + run(a_lo, b_hi))


NN = (((1,), (0,)), ((), ()))
NT = (((1,), (1,)), ((), ()))
BNN = (((2,), (1,)), ((0,), (0,)))
BNT = (((2,), (2,)), ((0,), (0,)))


def iota(shape, dim):
    return lax.broadcasted_iota(jnp.int32, shape, dim)


def delta_maps(recept, keys, values, learn, decay_log, passes):
    rows, width = recept.shape
    spans, heads = rows // SPAN, width // HEAD
    i, j = iota((rows, rows), 0), iota((rows, rows), 1)
    lower = ((i >> SPAN_BITS) == (j >> SPAN_BITS)) & (j <= i)
    lower = jnp.where(lower, 1.0, 0.0).astype(BF16)
    ones = head_ones(width)
    keys, values, recept = keys.astype(F32), values.astype(F32), recept.astype(F32)
    rate = jax.nn.sigmoid(learn.astype(F32))
    unit = keys * lax.rsqrt(dot(keys * keys, ones, NN, 2) + NORM_EPS)
    fall = -jnp.exp(decay_log)
    inclusive = sum(
        lax.dot_general(lower, part, NN, preferred_element_type=F32) for part in pieces(fall, 3)
    )
    last = jnp.concatenate(
        [
            jnp.broadcast_to(inclusive[(c + 1) * SPAN - 1 : (c + 1) * SPAN], (SPAN, width))
            for c in range(spans)
        ],
        axis=0,
    )
    shrunk = jnp.exp(-inclusive)
    tail = jnp.exp(last - inclusive)
    unit_rate = unit * rate

    def cut(x):
        return jnp.stack(
            [
                x[c * SPAN : (c + 1) * SPAN, h * HEAD : (h + 1) * HEAD]
                for c in range(spans)
                for h in range(heads)
            ]
        )

    def cut_turned(x):
        x = jnp.transpose(x)
        return jnp.stack(
            [
                x[h * HEAD : (h + 1) * HEAD, c * SPAN : (c + 1) * SPAN]
                for c in range(spans)
                for h in range(heads)
            ]
        )

    erase_in = cut(-unit * jnp.exp(inclusive - fall))
    read_in = cut(recept * jnp.exp(inclusive))
    erase_out, write_out = cut(unit_rate * shrunk), cut(keys * shrunk)
    value = cut(values)
    count = spans * heads
    zero = jnp.zeros((count, SPAN, HEAD), F32)

    i, j = iota((2 * SPAN, 2 * SPAN), 0), iota((2 * SPAN, 2 * SPAN), 1)
    allowed = (j & (SPAN - 1)) < (i & (SPAN - 1)) + (i >> SPAN_BITS)
    mixes = dot(
        jnp.concatenate([erase_in, read_in], 1),
        jnp.concatenate([erase_out, write_out], 1),
        BNT,
        passes,
    )
    mixes = jnp.where(allowed[None], mixes, 0.0)
    erase = mixes[:, :SPAN, :SPAN]
    i, j = iota((SPAN, SPAN), 0), iota((SPAN, SPAN), 1)

    def level(bit):
        same = (i >> (bit + 1)) == (j >> (bit + 1))
        return (same & (((i >> bit) & 1) == 1) & (((j >> bit) & 1) == 0))[None]

    inverse = jnp.where((i == j)[None], 1.0, jnp.where(level(0), erase, 0.0))
    for bit in range(1, SPAN_BITS):
        step = jnp.where(level(bit), erase, 0.0)
        inverse = inverse + dot(inverse, dot(step, inverse, BNN, passes), BNN, passes)
    mixed_values = dot(mixes, jnp.concatenate([zero, value], 1), BNN, passes)
    erased = dot(
        inverse, jnp.concatenate([erase_in, mixed_values[:, :SPAN]], 2), BNN, passes
    )
    outs = jnp.concatenate([read_in, mixed_values[:, SPAN:]], 2) + dot(
        mixes[:, SPAN:, :SPAN], erased, BNN, passes
    )
    turned = jnp.concatenate([cut_turned(unit_rate * tail), cut_turned(keys * tail)], 2)
    grow = jnp.exp(last)
    grow = jnp.concatenate([cut(grow), zero], 2)
    i, j = iota((HEAD, 2 * HEAD), 0), iota((HEAD, 2 * HEAD), 1)
    maps = dot(
        turned,
        jnp.concatenate([erased, jnp.concatenate([zero, value], 2)], 1),
        BNN,
        passes,
    ) + jnp.where((i == j)[None], grow, 0.0)
    right = (j >= HEAD)[None]
    before = maps[:heads]
    carried = [outs[:heads]]
    for c in range(1, spans):
        here = slice(c * heads, (c + 1) * heads)
        carried.append(
            dot(outs[here][:, :, :HEAD], before, BNN, passes) + jnp.where(right, outs[here], 0.0)
        )
        before = dot(maps[here][:, :, :HEAD], before, BNN, passes) + jnp.where(
            right, maps[here], 0.0
        )
    return jnp.concatenate(carried, 0), before


def head_ones(width):
    bits = HEAD.bit_length() - 1
    i, j = iota((width, width), 0), iota((width, width), 1)
    return jnp.where((i >> bits) == (j >> bits), 1.0, 0.0).astype(BF16)


def kernel(
    sizes, passes,
    q_in, k_in, v_in, f_in, fox_gain_ref,
    r_in, lk_in, lv_in, learn_in, decay_in, lin_gain_ref,
    wf_in, wl_in,
    out_ref,
    q_ref, r_ref, lk_ref, lv_ref, learn_ref, decay_ref,
    k_buf, v_buf, f_buf, map_own, map_buf, w_buf, carried_ref,
    max_ref, total_ref, acc_ref, act_ref, part_own, part_buf,
    k_send, v_send, f_send, k_recv, v_recv, f_recv,
    map_send, map_recv, w_send, w_recv, part_send, part_recv, local_sem,
):
    n_sp, n_fs, n_tp = sizes
    me, fs, tp = lax.axis_index("sp"), lax.axis_index("fs"), lax.axis_index("tp")
    rows, width = q_ref.shape
    heads = width // HEAD
    kv_heads = k_in.shape[1] // HEAD
    group = heads // kv_heads
    lin_heads = r_ref.shape[1] // HEAD
    spans = rows // SPAN
    lin_width = r_ref.shape[1]
    block = wf_in.shape[1]
    half = rows // n_tp

    targets = (
        (k_in, k_buf.at[me]), (v_in, v_buf.at[me]), (f_in, f_buf.at[me]),
        (wf_in, w_buf.at[fs, 0]), (wl_in, w_buf.at[fs, 1]),
        (decay_in, decay_ref), (lk_in, lk_ref), (learn_in, learn_ref),
        (r_in, r_ref), (lv_in, lv_ref), (q_in, q_ref),
    )
    loads = [
        pltpu.make_async_copy(src, dst, local_sem.at[at]) for at, (src, dst) in enumerate(targets)
    ]
    for load in loads:
        load.start()

    barrier = pltpu.get_barrier_semaphore()

    def greet(step, _):
        pl.semaphore_signal(
            barrier, inc=1, device_id={"sp": lax.rem(me + step, n_sp)}, device_id_type=MESH
        )
        return 0

    lax.fori_loop(1, n_sp, greet, 0)
    for step in range(1, n_fs):
        pl.semaphore_signal(
            barrier, inc=1, device_id={"fs": lax.rem(fs + step, n_fs)}, device_id_type=MESH
        )
    for step in range(1, n_tp):
        pl.semaphore_signal(
            barrier, inc=1, device_id={"tp": lax.rem(tp + step, n_tp)}, device_id_type=MESH
        )
    pl.semaphore_wait(barrier, n_sp + n_fs + n_tp - 3)

    def map_copy(source, other):
        return pltpu.make_async_remote_copy(
            src_ref=map_own, dst_ref=map_buf.at[source],
            send_sem=map_send.at[other], recv_sem=map_recv.at[source],
            device_id={"sp": other}, device_id_type=MESH,
        )

    def block_copy(item, source, hop):
        buf, send, recv = item
        return pltpu.make_async_remote_copy(
            src_ref=buf.at[source], dst_ref=buf.at[source],
            send_sem=send.at[source, hop - 1], recv_sem=recv.at[source],
            device_id={"sp": lax.rem(me + hop, n_sp)}, device_id_type=MESH,
        )

    shared = ((k_buf, k_send, k_recv), (v_buf, v_send, v_recv), (f_buf, f_send, f_recv))

    def on_block(source, act):
        for hop in (1, 2):
            if hop < n_sp:

                @pl.when(me + hop < n_sp)
                def _():
                    for item in shared:
                        act(block_copy(item, source, hop))

    for load in loads[:3]:
        load.wait()
    on_block(me, lambda copy: copy.start())

    def weight_copy(which, source, step, target):
        return pltpu.make_async_remote_copy(
            src_ref=w_buf.at[source, which], dst_ref=w_buf.at[source, which],
            send_sem=w_send.at[which, step], recv_sem=w_recv.at[which, source],
            device_id={"fs": target}, device_id_type=MESH,
        )

    relayed = n_fs == 4
    if relayed:
        beside = fs + 1 - 2 * lax.rem(fs, 2)
        across = lax.rem(fs + 2, 4)
        direct = [
            weight_copy(0, fs, 0, beside), weight_copy(1, fs, 0, across),
            weight_copy(1, fs, 1, beside), weight_copy(0, fs, 1, across),
        ]
        passed = [weight_copy(0, beside, 2, across), weight_copy(1, across, 2, beside)]
        order = [fs, beside, across, lax.rem(beside + 2, 4)]
    else:
        direct = [
            weight_copy(which, fs, step - 1, lax.rem(fs + step, n_fs))
            for which in range(2)
            for step in range(1, n_fs)
        ]
        passed = []
        order = [lax.rem(fs + step, n_fs) for step in range(n_fs)]
    for load in loads[3:5]:
        load.wait()
    for copy in direct:
        copy.start()
    for load in loads[5:]:
        load.wait()

    carried, maps = delta_maps(
        r_ref[...], lk_ref[...], lv_ref[...], learn_ref[...], decay_ref[...], passes
    )
    map_own[...] = maps.astype(BF16)
    carried_ref[...] = carried

    def send_map(other, _):
        map_copy(me, other).start()
        return 0

    lax.fori_loop(me + 1, n_sp, send_map, 0)

    for copy in passed:
        copy.wait_recv()
        copy.start()

    scaled = (q_ref[...].astype(F32) * HEAD ** (-0.5)).astype(BF16)

    def attend(key_block, value_block, forget_block, first):
        pad = jnp.zeros((-heads % 8, rows), F32)
        forget = jnp.transpose(jnp.concatenate([forget_block, pad], axis=0))
        turned = jnp.transpose(value_block)
        if first:
            seen = iota((rows, rows), 0) <= iota((rows, rows), 1)
        for h in range(heads):
            kv = slice(h // group * HEAD, (h // group + 1) * HEAD)
            scores = lax.dot_general(
                key_block[:, kv], scaled[:, h * HEAD : (h + 1) * HEAD], NT,
                preferred_element_type=F32,
            ) - forget[:, h : h + 1]
            if first:
                scores = jnp.where(seen, scores, -1e30)
            top = jnp.max(scores, axis=0, keepdims=True)
            if not first:
                old = max_ref[h]
                top = jnp.maximum(old, top)
                rescale = jnp.exp(old - top)
            weights = jnp.exp(scores - top)
            total = jnp.sum(weights, axis=0, keepdims=True)
            update = lax.dot_general(
                turned[kv], weights.astype(BF16), NN, preferred_element_type=F32
            )
            if not first:
                total = total + total_ref[h] * rescale
                update = update + acc_ref[h] * rescale
            max_ref[h] = top
            total_ref[h] = total
            acc_ref[h] = update

    attend(k_buf[me], v_buf[me], f_buf[me], True)

    def pass_on(step, _):
        source = me - 2 * step
        for item in shared:
            block_copy(item, source, 1).wait_recv()
        on_block(source, lambda copy: copy.start())
        return 0

    lax.fori_loop(1, me // 2 + 1, pass_on, 0)

    def earlier(step, _):
        other = me - 1 - step

        @pl.when(lax.rem(step, 2) == 0)
        def _():
            for item in shared:
                block_copy(item, other, 1).wait_recv()

        attend(k_buf[other], v_buf[other], f_buf[other], False)
        return 0

    lax.fori_loop(0, me, earlier, 0)
    normed = []
    for h in range(heads):
        attended = acc_ref[h] / total_ref[h]
        normed.append(
            attended
            * lax.rsqrt(jnp.mean(attended * attended, axis=0, keepdims=True) + NORM_EPS)
        )
    fox_out = jnp.transpose(jnp.concatenate(normed, axis=0)) * fox_gain_ref[...]
    act_ref[:, :width] = fox_out.astype(BF16)

    def join(other, state):
        map_copy(other, other).wait_recv()
        step = map_buf[other]
        return dot(step[:, :, :HEAD].astype(F32), state, BNN, passes) + step[:, :, HEAD:].astype(F32)

    state = lax.fori_loop(0, me, join, jnp.zeros((lin_heads, HEAD, HEAD), F32))
    eye = jnp.where(iota((HEAD, HEAD), 0) == iota((HEAD, HEAD), 1), 1.0, 0.0)
    eye = jnp.broadcast_to(eye[None], (lin_heads, HEAD, HEAD))
    state = jnp.concatenate([state, eye], axis=1)
    read = []
    for c in range(spans):
        here = dot(carried_ref[c * lin_heads : (c + 1) * lin_heads], state, BNN, 3)
        read.append(jnp.concatenate([here[h] for h in range(lin_heads)], axis=1))
    read = jnp.concatenate(read, axis=0)
    ones = head_ones(lin_width)
    centred = read - dot(read, ones, NN, 2) * (1.0 / HEAD)
    spread = dot(centred * centred, ones, NN, 2) * (1.0 / HEAD)
    lin_out = centred * lax.rsqrt(spread + HEAD * 1e-05) * lin_gain_ref[...]
    act_ref[:, width:] = lin_out.astype(BF16)

    def project(first, source):
        act = act_ref[pl.ds(pl.multiple_of(first, half), half), :]
        return lax.dot_general(
            act[:, :width], w_buf[source, 0], NN, preferred_element_type=F32
        ) + lax.dot_general(act[:, width:], w_buf[source, 1], NN, preferred_element_type=F32)

    def part_copy(step, source):
        return pltpu.make_async_remote_copy(
            src_ref=part_own.at[step - 1, source], dst_ref=part_buf.at[step - 1, source],
            send_sem=part_send.at[step - 1, source], recv_sem=part_recv.at[step - 1, source],
            device_id={"tp": lax.rem(tp + step, n_tp)}, device_id_type=MESH,
        )

    for hop, source in enumerate(order):
        for which in range(2):
            if hop > 0 and not (relayed and which == hop - 1):
                weight_copy(which, source, 0, source).wait_recv()
        for step in range(1, n_tp):
            part_own[step - 1, source] = project(
                lax.rem(tp + step, n_tp) * half, source
            ).astype(BF16)
            part_copy(step, source).start()
    for source in range(n_fs):
        total = project(tp * half, source).astype(BF16).astype(F32)
        for step in range(1, n_tp):
            part_copy(step, source).wait_recv()
            total = total + part_buf[step - 1, source].astype(F32)
        out_ref[:, source * block : (source + 1) * block] = total

    def drain(other, _):
        map_copy(me, other).wait_send()
        return 0

    lax.fori_loop(me + 1, n_sp, drain, 0)

    def drain_blocks(step, _):
        on_block(me - 2 * step, lambda copy: copy.wait_send())
        return 0

    lax.fori_loop(0, me // 2 + 1, drain_blocks, 0)
    for copy in direct + passed:
        copy.wait_send()
    for source in range(n_fs):
        for step in range(1, n_tp):
            part_copy(step, source).wait_send()


def shards(
    sizes, passes,
    queries, keys, values, forget_cache, fox_gain, receptance, lin_keys, lin_values,
    learn_logit, decay_log, lin_gain, out_fox_weight, out_lin_weight,
):
    n_sp, n_fs, n_tp = sizes
    _, rows, width = queries.shape
    kv_width = keys.shape[2]
    lin_width = receptance.shape[2]
    heads, lin_heads = width // HEAD, lin_width // HEAD
    fox_rows, block = out_fox_weight.shape
    half = rows // n_tp
    forget = jnp.transpose(forget_cache[0])
    dma = pltpu.SemaphoreType.DMA
    vmem = pltpu.VMEM
    near = pl.BlockSpec(memory_space=vmem)
    anywhere = pl.BlockSpec(memory_space=pl.ANY)
    out = pl.pallas_call(
        functools.partial(kernel, sizes, passes),
        out_shape=jax.ShapeDtypeStruct((half, n_fs * block), F32),
        in_specs=[anywhere] * 4 + [near] + [anywhere] * 5 + [near] + [anywhere] * 2,
        out_specs=pl.BlockSpec(memory_space=vmem),
        scratch_shapes=[vmem((rows, width), BF16)]
        + [vmem((rows, lin_width), BF16)] * 4
        + [vmem((rows, lin_width), F32)]
        + [
            vmem((n_sp, rows, kv_width), BF16),
            vmem((n_sp, rows, kv_width), BF16),
            vmem((n_sp,) + forget.shape, F32),
            vmem((lin_heads, HEAD, 2 * HEAD), BF16),
            vmem((n_sp, lin_heads, HEAD, 2 * HEAD), BF16),
            vmem((n_fs, 2, fox_rows, block), BF16),
            vmem((rows // SPAN * lin_heads, SPAN, 2 * HEAD), F32),
            vmem((heads, 1, rows), F32),
            vmem((heads, 1, rows), F32),
            vmem((heads, HEAD, rows), F32),
            vmem((rows, width + lin_width), BF16),
            vmem((n_tp - 1, n_fs, half, block), BF16),
            vmem((n_tp - 1, n_fs, half, block), BF16),
        ]
        + [dma((n_sp, 2))] * 3
        + [dma((n_sp,))] * 5
        + [dma((2, n_fs))] * 2
        + [dma((n_tp - 1, n_fs))] * 2
        + [dma((11,))],
        compiler_params=pltpu.CompilerParams(
            collective_id=0, has_side_effects=True, vmem_limit_bytes=60 * 1024 * 1024
        ),
    )(
        queries[0], keys[0], values[0], forget, fox_gain[None],
        receptance[0], lin_keys[0], lin_values[0], learn_logit[0], decay_log[0], lin_gain[None],
        out_fox_weight, out_lin_weight,
    )
    return out.astype(BF16)[None]


def solution(mesh, passes=3):
    sizes = tuple(mesh.shape[name] for name in ("sp", "fs", "tp"))
    rows = P("fs", "sp", "tp")
    return jax.shard_map(
        functools.partial(shards, sizes, passes),
        mesh=mesh,
        in_specs=(rows,) * 4 + (P("tp"),) + (rows,) * 5 + (P("tp"), P("tp", "fs"), P("tp", "fs")),
        out_specs=P("fs", ("sp", "tp"), None),
        check_vma=False,
    )
```
